32 devices in a mesh: sp: 8 (over z, core), tp: 4 (over y, x).
Axes of the slice: x: 2, y: 2, z: 4, core: 2. Of those that a mesh axis runs over, the one named last changes fastest.
Arguments:
- stream: bfloat16 [3072, 2048], P('sp'), may hold values from -6 to 6
- inner_act: bfloat16 [3072, 4096], P('sp', 'tp'), may hold values from -6 to 6
- gate_act: bfloat16 [3072, 4096], P('sp', 'tp'), may hold values from -6 to 6
- state_write: bfloat16 [3072, 16, 128], P('sp', 'tp'), may hold values from -6 to 6
- state_read: bfloat16 [3072, 16, 128], P('sp', 'tp'), may hold values from -6 to 6
- step_raw: bfloat16 [3072, 64], P('sp', 'tp'), may hold values from -4.6 to 4.1
- conv_inner: bfloat16 [4, 4096], P(None, 'tp'), may hold values from -3 to 3
- conv_write: bfloat16 [4, 16, 128], P(None, 'tp'), may hold values from -3 to 3
- conv_read: bfloat16 [4, 16, 128], P(None, 'tp'), may hold values from -3 to 3
- step_bias: float32 [64], P('tp'), may hold values from -0.5 to 0.5
- decay_log: float32 [64], P('tp'), may hold values from -13 to -2.52, as said below
- inner_gain: float32 [4096], P('tp'), may hold values from 0.1 to 1.9
- out_weight: bfloat16 [4096, 2048], P('tp'), may hold values from -0.09375 to 0.09375
- ffn_gain: float32 [2048], replicated, may hold values from 0.1 to 1.9
- expert_ids: int32 [3072, 2], P('sp'), may hold values from 0 to 31, all different within a row; in each aligned block of 384 rows (0 to 383, 384 to 767, ...) at most 48 rows name the same one
- expert_weights: float32 [3072, 2], P('sp'), may hold values from 0.1 to 1
- expert_gate: bfloat16 [32, 2048, 1024], P('sp', None, 'tp'), may hold values from -0.125 to 0.125
- expert_up: bfloat16 [32, 2048, 1024], P('sp', None, 'tp'), may hold values from -0.125 to 0.125
- expert_down: bfloat16 [32, 1024, 2048], P('sp', None, 'tp'), may hold values from -0.1875 to 0.1875
Outputs:
- layer_out: bfloat16 [3072, 2048], P('sp', 'tp')
The draws below stay inside these ranges and needn't reach their ends.
Inputs may be any that keep to these rules, and one draw needn't show every extreme that they name: The logarithm of a per-position decay rate: exp(decay_log) lies between 0.1 / 3072 and 0.08. `expert_ids`: each row names 2 different experts. Among the rows of one index of sp (384 tokens) no expert is named more than 48 times, a bound that some block reaches there.
All inputs are finite; a program needn't handle non-finite values.
Results may differ from the reference program's by a relative error of at most 0.014.
Values may be sent and summed in bfloat16 or wider, within the bound.
A program may use at most 64 MiB of HBM per device.

```python
import math
import jax
import jax.numpy as jnp
import numpy as np
from jax import lax

D = 2048
HEADS = 64
HEADDIM = 64
GROUPS = 16
STATE = 128
CONV = 4
BLOCK = 64
FF = 1024
EXPERTS = 32
TOPK = 2
TOK_SP = 384
D_INNER = 4096
TOKENS = 3072
CAP = 48
N_SP = 8
N_TP = 4


def draw_step_raw(key, part):
    key_noise, key_device, key_block = jax.random.split(jax.random.fold_in(key, 11), 3)
    jitter = 0.7 * jax.random.truncated_normal(key_noise, -3.0, 3.0, (TOKENS, HEADS), jnp.float32)
    device_shift = jax.random.uniform(key_device, (TOKENS // TOK_SP, 1, HEADS), jnp.float32, -2.0, 1.5)
    block_shift = jax.random.uniform(key_block, (TOKENS // BLOCK, 1, HEADS), jnp.float32, -0.5, 0.5)
    shifted = jitter.reshape(TOKENS // TOK_SP, TOK_SP, HEADS) + device_shift
    shifted = shifted.reshape(TOKENS // BLOCK, BLOCK, HEADS) + block_shift
    return shifted.reshape(TOKENS, HEADS).astype(jnp.bfloat16)


def draw_decay_log(key, part):
    key_pick, key_level = jax.random.split(jax.random.fold_in(key, 23))
    slow_share = 0.5
    slower = jax.random.bernoulli(key_pick, slow_share, (HEADS,))
    level = jax.random.uniform(key_level, (HEADS,), jnp.float32)
    slow_log = math.log(0.1) + level * math.log(5.0) - math.log(TOKENS)
    fast_log = math.log(0.02) + level * math.log(4.0)
    return jnp.where(slower, slow_log, fast_log).astype(jnp.float32)


def level_of(key, extent, cuts, smallest, high):
    gain, own = 1.0, jax.random.fold_in(key, 6)
    for dim, shards_of in cuts:
        steps = jnp.exp(jax.random.uniform(jax.random.fold_in(own, dim), (shards_of,), jnp.float32, smallest / len(cuts), high / len(cuts)))
        gain = gain * jnp.repeat(steps, extent[dim] // shards_of).reshape([-1 if axis == dim else 1 for axis in range(len(extent))])
    return gain


def routed_block(rng, own, number, rows, count, top, bound, skew):
    order = jax.random.permutation(rng, count)
    packed, ordinary = shares(count, rows * top, bound, skew, True), shares(count, rows * top, bound, skew, False)
    places = jnp.arange(count)

    def named(tallies, rotation):
        used = int((tallies > 0).sum())
        fixed = max(1, used // 4)
        passed = fixed + (places - fixed + rotation * (used - fixed)) % max(1, count - fixed)
        return jnp.zeros((count,), jnp.int32).at[order[jnp.where(places < fixed, places, passed)]].set(jnp.asarray(tallies, jnp.int32))

    tallies = jnp.where(number % 4 == 0, named(packed, number // 4), named(ordinary, number - number // 4 - 1))
    mixed = jax.random.permutation(jax.random.fold_in(own, 3), count)
    donor, receiver = mixed[0:count // 2 * 2:2], mixed[1:count // 2 * 2:2]
    room = jnp.minimum(tallies[donor] - 1, bound - tallies[receiver]) // 2
    room = jnp.where((donor == order[0]) | (receiver == order[0]) | (tallies[receiver] == 0), 0, jnp.maximum(room, 0))
    passed = jax.random.randint(jax.random.fold_in(own, 4), (count // 2,), 0, 1 << 20) % (room + 1)
    tallies = tallies.at[donor].add(-passed).at[receiver].add(passed)
    members = jnp.searchsorted(jnp.cumsum(tallies), jnp.arange(rows * top), side="right").astype(jnp.int32)
    listing = members.reshape(top, rows).T
    listing = listing[jax.random.permutation(jax.random.fold_in(own, 1), rows)]
    rotation = jax.random.randint(jax.random.fold_in(own, 2), (rows, 1), 0, top)
    return jnp.take_along_axis(listing, (jnp.arange(top)[None, :] + rotation) % top, axis=1)


def shares(count, total, bound, slope, full):
    weights = [(1 << 20) // math.isqrt(standing ** slope) + 1 for standing in range(1, count + 1)]
    largest = bound if full else min(bound, max(-(-total // count), total * weights[0] // sum(weights)))
    least = 1 if total - largest >= count - 1 else 0
    holding, rest = [largest] + [least] * (count - 1), total - largest - least * (count - 1)
    while rest > 0:
        candidates = [i for i in range(1, count) if holding[i] < largest] or [i for i in range(1, count) if holding[i] < bound]
        whole, budget = sum([weights[i] for i in candidates]), rest
        for i in candidates:
            extra = min(bound - holding[i], max(1, budget * weights[i] // whole), rest)
            holding[i] = holding[i] + extra
            rest = rest - extra
    return np.array(holding)


def centred(stream_key, shape, scale, limit, shards=(), held_as=jnp.bfloat16):
    loudness = level_of(stream_key, shape, shards, -0.22, 0.18) if shards else 1.0
    result = jax.random.normal(stream_key, shape, jnp.float32) * scale * loudness
    return jnp.minimum(jnp.maximum(result, -limit), limit).astype(held_as)


def setup_inputs(seed: int = 0) -> dict:
    seeds = jax.random.split(jax.random.key(seed), 20)
    stream = centred(seeds[0], (TOKENS, D), 1.0, 6.0, ((0, 8),))
    inner_act = centred(seeds[1], (TOKENS, D_INNER), 1.0, 6.0, ((0, 8), (1, 4)))
    gate_act = centred(seeds[2], (TOKENS, D_INNER), 1.0, 6.0, ((0, 8), (1, 4)))
    state_write = centred(seeds[3], (TOKENS, GROUPS, STATE), 1.0, 6.0, ((0, 8), (1, 4)))
    state_read = centred(seeds[4], (TOKENS, GROUPS, STATE), 1.0, 6.0, ((0, 8), (1, 4)))
    step_raw = draw_step_raw(jax.random.fold_in(seeds[19], 71), 0)
    conv_inner = centred(seeds[6], (CONV, D_INNER), 0.5, 3.0, ((1, 4),))
    conv_write = centred(seeds[7], (CONV, GROUPS, STATE), 0.5, 3.0, ((1, 4),))
    conv_read = centred(seeds[8], (CONV, GROUPS, STATE), 0.5, 3.0, ((1, 4),))
    step_bias = jnp.clip(jax.random.uniform(seeds[9], (HEADS,), jnp.float32, -0.5, 0.5) * level_of(seeds[9], (HEADS,), ((0, 4),), -0.4, 0.0), -0.5, 0.5)
    decay_log = draw_decay_log(jax.random.fold_in(seeds[19], 71), 0)
    inner_gain = jnp.clip(1.0 + 0.18 * jax.random.normal(seeds[11], (D_INNER,), jnp.float32), 0.1, 1.9)
    out_weight = centred(seeds[12], (D_INNER, D), D_INNER ** -0.5, 0.09375, ((0, 4),))
    ffn_gain = jnp.clip(1.0 + 0.18 * jax.random.normal(seeds[13], (D,), jnp.float32), 0.1, 1.9)
    expert_ids_keys = jax.random.split(jax.random.fold_in(seeds[14], 1), TOKENS // TOK_SP)
    expert_ids_turns = jax.random.permutation(jax.random.fold_in(seeds[14], 3), TOKENS // TOK_SP)
    expert_ids = jax.vmap(lambda own, number: routed_block(jax.random.fold_in(seeds[14], 2), own, number, TOK_SP, EXPERTS, TOPK, CAP, 1))(expert_ids_keys, expert_ids_turns).reshape((TOKENS, TOPK))
    expert_weights = jnp.clip(0.1 + 0.9 * jax.random.uniform(seeds[15], (TOKENS, TOPK), jnp.float32) ** level_of(seeds[15], (TOKENS, TOPK), ((0, 8),), -0.2, 0.2), 0.1, 1.0)
    expert_gate = centred(seeds[16], (EXPERTS, D, FF), D ** -0.5, 0.125, ((0, 8), (2, 4)))
    expert_up = centred(seeds[17], (EXPERTS, D, FF), D ** -0.5, 0.125, ((0, 8), (2, 4)))
    expert_down = centred(seeds[18], (EXPERTS, FF, D), FF ** -0.5, 0.1875, ((0, 8), (2, 4)))
    return {"stream": stream, "inner_act": inner_act, "gate_act": gate_act, "state_write": state_write, "state_read": state_read, "step_raw": step_raw, "conv_inner": conv_inner, "conv_write": conv_write, "conv_read": conv_read, "step_bias": step_bias, "decay_log": decay_log, "inner_gain": inner_gain, "out_weight": out_weight, "ffn_gain": ffn_gain, "expert_ids": expert_ids, "expert_weights": expert_weights, "expert_gate": expert_gate, "expert_up": expert_up, "expert_down": expert_down}


HIGH = lax.Precision.HIGHEST
EPS = 1e-06

def conv_silu(padded, weights, length):
    running = jnp.zeros((length, padded.shape[1]), jnp.float32)
    for offset in range(weights.shape[0]):
        running = running + weights[offset][None, :] * padded[offset:offset + length]
    return jax.nn.silu(running)

def block_terms(values, step_len, decay_rate, writes, reads, block_len):
    blocks = values.shape[0] // block_len
    groups, per_group, head_dim = (values.shape[1], values.shape[2], values.shape[3])
    state_dim = writes.shape[2]
    value_blk = values.reshape(blocks, block_len, groups, per_group, head_dim)
    step_blk = step_len.reshape(blocks, block_len, groups, per_group)
    write_blk = writes.reshape(blocks, block_len, groups, state_dim)
    read_blk = reads.reshape(blocks, block_len, groups, state_dim)
    cumul = jnp.cumsum(step_blk * decay_rate, axis=1)
    causal = jnp.tril(jnp.ones((block_len, block_len), dtype=bool))[None, :, :, None, None]
    spread = cumul[:, :, None] - cumul[:, None, :]
    within = jnp.where(causal, jnp.exp(jnp.where(causal, spread, 0.0)), 0.0)
    intersect = jnp.einsum('clgn,csgn->clsg', read_blk, write_blk, precision=HIGH)
    mixing = intersect[..., None] * within * step_blk[:, None]
    inside = jnp.einsum('clsgh,csghp->clghp', mixing, value_blk, precision=HIGH)
    to_end = jnp.exp(cumul[:, -1:] - cumul) * step_blk
    block_state = jnp.einsum('clgn,clghp->cghpn', write_blk, to_end[..., None] * value_blk, precision=HIGH)
    block_decay = jnp.exp(cumul[:, -1])

    def advance(carried, inputs):
        state_here, decay_here = inputs
        return (carried * decay_here[..., None, None] + state_here, carried)
    initial = jnp.zeros(block_state.shape[1:], jnp.float32)
    closing, entering = lax.scan(advance, initial, (block_state, block_decay))
    return (inside, entering, cumul, read_blk, closing)

def convolve(source, kernel):
    channels = source.shape[1]
    padded = jnp.concatenate([jnp.zeros((CONV - 1, channels), jnp.float32), source.astype(jnp.float32)], axis=0)
    return conv_silu(padded, kernel.astype(jnp.float32).reshape(CONV, channels), TOKENS)

def reference(stream, inner_act, gate_act, state_write, state_read, step_raw, conv_inner, conv_write, conv_read, step_bias, decay_log, inner_gain, out_weight, ffn_gain, expert_ids, expert_weights, expert_gate, expert_up, expert_down):
    per_group = HEADS // GROUPS
    write_width = GROUPS * STATE
    values = convolve(inner_act, conv_inner).reshape(TOKENS, GROUPS, per_group, HEADDIM)
    writes = convolve(state_write.reshape(TOKENS, write_width), conv_write).reshape(TOKENS, GROUPS, STATE)
    reads = convolve(state_read.reshape(TOKENS, write_width), conv_read).reshape(TOKENS, GROUPS, STATE)
    step_len = jax.nn.softplus(step_raw.astype(jnp.float32) + step_bias[None, :]).reshape(TOKENS, GROUPS, per_group)
    decay_rate = (-jnp.exp(decay_log)).reshape(GROUPS, per_group)
    inside, entering, cumul, read_blk, closing = block_terms(values, step_len, decay_rate, writes, reads, BLOCK)
    outside = jnp.einsum('clgn,cghpn->clghp', read_blk, entering, precision=HIGH) * jnp.exp(cumul)[..., None]
    gated = (inside + outside).reshape(TOKENS, D_INNER) * jax.nn.silu(gate_act.astype(jnp.float32))
    per_head = gated.reshape(TOKENS, HEADS, HEADDIM)
    per_head = per_head * lax.rsqrt(lax.optimization_barrier(jnp.mean(per_head * per_head, axis=-1, keepdims=True)) + EPS)
    mixed_inner = (per_head.reshape(TOKENS, D_INNER) * inner_gain[None, :]).astype(jnp.bfloat16)
    block_width = D_INNER // N_TP

    def add_block(index, running):
        begin = (index * block_width).astype(jnp.int32)
        columns = lax.dynamic_slice_in_dim(mixed_inner, begin, block_width, 1)
        weight_rows = lax.dynamic_slice_in_dim(out_weight, begin, block_width, 0)
        partial_value = jnp.dot(columns, weight_rows, preferred_element_type=jnp.float32).astype(jnp.bfloat16)
        partial_value = lax.optimization_barrier(partial_value)
        return running + partial_value.astype(jnp.float32)
    projected = lax.fori_loop(0, N_TP, add_block, jnp.zeros((TOKENS, D), jnp.float32))
    middle = stream.astype(jnp.float32) + projected
    normed = (middle * lax.rsqrt(lax.optimization_barrier(jnp.mean(middle * middle, axis=-1, keepdims=True)) + EPS) * ffn_gain[None, :]).astype(jnp.bfloat16)
    per_block = TOK_SP * TOPK
    choices_blk = expert_ids.reshape(N_SP, per_block)
    onehot = (choices_blk[..., None] == jnp.arange(EXPERTS, dtype=jnp.int32)[None, None, :]).astype(jnp.int32)
    earlier_count = jnp.cumsum(onehot, axis=1) - onehot
    slot_of = lax.optimization_barrier(jnp.sum(earlier_count * onehot, axis=-1))
    owner = jnp.arange(N_SP, dtype=jnp.int32)[:, None]
    target = (choices_blk * (N_SP * CAP) + owner * CAP + slot_of).reshape(-1).astype(jnp.int32)
    token_of = (jnp.arange(TOKENS * TOPK, dtype=jnp.int32) // TOPK).astype(jnp.int32)
    slot_table = jnp.full((EXPERTS * N_SP * CAP,), TOKENS, jnp.int32).at[target].set(token_of)
    slot_table = slot_table.reshape(EXPERTS, N_SP * CAP)
    padded_rows = jnp.concatenate([normed, jnp.zeros((1, D), jnp.bfloat16)], axis=0)

    def one_expert(index):
        tok_rows = padded_rows[slot_table[index]]
        gate_part = jnp.dot(tok_rows, expert_gate[index], preferred_element_type=jnp.float32)
        up_part = jnp.dot(tok_rows, expert_up[index], preferred_element_type=jnp.float32)
        hidden = (jax.nn.silu(gate_part) * up_part).astype(jnp.bfloat16)
        return jnp.dot(hidden, expert_down[index], preferred_element_type=jnp.float32).astype(jnp.bfloat16)
    results = lax.map(one_expert, jnp.arange(EXPERTS, dtype=jnp.int32))
    results = results.reshape(EXPERTS * N_SP * CAP, D)
    picked = results[target].astype(jnp.float32).reshape(TOKENS, TOPK, D)
    moe = lax.optimization_barrier(jnp.sum(picked * expert_weights[:, :, None], axis=1))
    return (middle + moe).astype(jnp.bfloat16)
```

```python
import functools

import jax
import jax.numpy as jnp
from jax import lax
from jax.experimental import pallas as pl
from jax.experimental.pallas import tpu as pltpu
from jax.sharding import PartitionSpec as P

TOPK = 2
CAP = 48
EPS = 1e-06
HIGH = lax.Precision.HIGHEST
MESH = pl.DeviceIdType.MESH
HALO = 8
VMEM = pl.BlockSpec(memory_space=pltpu.VMEM)
ANY = pl.BlockSpec(memory_space=pl.ANY)
F32 = jnp.float32
BF16 = jnp.bfloat16


def silu(x):
    return x / (1.0 + jnp.exp(-x))


def nt_dot(a, b):
    return lax.dot_general(a, b, (((1,), (1,)), ((), ())), preferred_element_type=F32)


def tn_dot(a, b):
    return lax.dot_general(a, b, (((0,), (0,)), ((), ())), preferred_element_type=F32)


def conv_kernel(
    per_group, x_ref, w_ref, r_ref, hx_ref, hw_ref, hr_ref, kx_ref, kw_ref, kr_ref, end_ref,
    xs_ref, bw_ref, cr_ref, state_ref, pad_ref,
):
    length = x_ref.shape[0]

    def conv(src_ref, halo_ref, tap_ref):
        width = src_ref.shape[1]
        pad_ref[0:HALO, 0:width] = halo_ref[...].astype(F32)
        pad_ref[HALO : HALO + length, 0:width] = src_ref[...].astype(F32)
        taps = tap_ref[...].astype(F32)
        count = taps.shape[0]
        total = jnp.zeros((length, width), F32)
        for k in range(count):
            begin = HALO + k - count + 1
            total = total + taps[k : k + 1, :] * pad_ref[begin : begin + length, 0:width]
        return silu(total)

    xs = conv(x_ref, hx_ref, kx_ref)
    bw = conv(w_ref, hw_ref, kw_ref).astype(BF16)
    cr_ref[...] = conv(r_ref, hr_ref, kr_ref).astype(BF16)
    xs_ref[...] = xs.astype(BF16)
    bw_ref[...] = bw
    head_dim = xs.shape[1] // per_group
    scaled = [
        xs[:, h * head_dim : (h + 1) * head_dim] * end_ref[0, :, h : h + 1] for h in range(per_group)
    ]
    weighted = jnp.concatenate(scaled, axis=1).astype(BF16)
    state_ref[...] = tn_dot(weighted, bw).astype(BF16)


def inside_kernel(per_group, xs_ref, bw_ref, cr_ref, cum_ref, cumt_ref, stept_ref, out_ref):
    length = xs_ref.shape[0]
    head_dim = xs_ref.shape[1] // per_group
    scores = nt_dot(cr_ref[...], bw_ref[...])
    rows = lax.broadcasted_iota(jnp.int32, (length, length), 0)
    columns = lax.broadcasted_iota(jnp.int32, (length, length), 1)
    causal = rows >= columns
    pieces = []
    for h in range(per_group):
        spread = cum_ref[0, :, h : h + 1] - cumt_ref[0, h : h + 1, :]
        within = jnp.exp(jnp.where(causal, spread, -1e30))
        mixing = (scores * within * stept_ref[0, h : h + 1, :]).astype(BF16)
        pieces.append(
            jnp.dot(
                mixing, xs_ref[:, h * head_dim : (h + 1) * head_dim], preferred_element_type=F32
            )
        )
    out_ref[...] = jnp.concatenate(pieces, axis=1)


def outside_kernel(
    per_group, in_ref, cr_ref, state_ref, cum_ref, gate_ref, gain_ref, out_ref
):
    head_dim = in_ref.shape[1] // per_group
    outside = nt_dot(cr_ref[...], state_ref[...])
    gates = silu(gate_ref[...].astype(F32))
    pieces = []
    for h in range(per_group):
        cut = slice(h * head_dim, (h + 1) * head_dim)
        part = in_ref[:, cut] + outside[:, cut] * jnp.exp(cum_ref[0, :, h : h + 1])
        part = part * gates[:, cut]
        scale = lax.rsqrt(jnp.mean(part * part, axis=1, keepdims=True) + EPS)
        pieces.append(part * scale)
    out_ref[...] = (jnp.concatenate(pieces, axis=1) * gain_ref[...]).astype(BF16)


def experts_kernel(
    n_sp, n_tp, slots_ref, gate_hbm, up_hbm, down_hbm, back_ref,
    gate_ref, up_ref, down_ref, rows_ref, hid_ref, done_ref,
    w_sem, own_sem, s_send, s_recv, x_send, x_recv, y_send, y_recv, dx_send, dx_recv, dy_send, dy_recv,
    hx_send, hx_recv, hy_send, hy_recv, hdx_send, hdx_recv, hdy_send, hdy_recv, r_send, r_recv,
):
    me = lax.axis_index("sp")
    tp = lax.axis_index("tp")
    plane, core = me // 2, me % 2
    planes = n_sp // 2
    xp = tp + 1 - 2 * (tp % 2)
    yp = (tp + 2) % 4
    experts = gate_ref.shape[0]
    half = experts // 2
    cap = rows_ref.shape[3]
    share = rows_ref.shape[4]
    width = hid_ref.shape[4]

    barrier = pltpu.get_barrier_semaphore()
    for step in range(1, n_sp):
        pl.semaphore_signal(
            barrier, inc=1, device_id=((me + step) % n_sp, tp), device_id_type=MESH
        )
    for peer in (xp, yp):
        pl.semaphore_signal(barrier, inc=1, device_id=(me, peer), device_id_type=MESH)
    pl.semaphore_wait(barrier, n_sp + 1)

    sends = []

    def remote(src, dst, send, recv, device):
        return pltpu.make_async_remote_copy(
            src_ref=src, dst_ref=dst, send_sem=send, recv_sem=recv,
            device_id=device, device_id_type=MESH,
        )

    def start(copy):
        copy.start()
        sends.append(copy)

    own = pltpu.make_async_copy(slots_ref.at[me], rows_ref.at[tp, me], own_sem.at[0])
    own.start()
    for j in range(planes):
        for c in range(2):
            if j == 0 and c == 1:
                continue
            to_core = (core + 1) % 2 if j == 0 else c
            target = ((plane - j + planes) % planes) * 2 + to_core
            start(
                remote(
                    slots_ref.at[target], rows_ref.at[tp, me], s_send.at[j * 2 + c],
                    s_recv.at[j * 2 + core], (target, tp),
                )
            )
    loads = [
        pltpu.make_async_copy(a, b, w_sem.at[i])
        for i, (a, b) in enumerate(
            ((gate_hbm, gate_ref), (up_hbm, up_ref), (down_hbm, down_ref))
        )
    ]
    for load in loads:
        load.start()

    def source(j, c):
        return ((plane + j) % planes) * 2 + c

    def exchange(buf, j, c, sems):
        s = source(j, c)
        k = j * 2 + c
        piece = buf.at[tp, s]
        start(remote(piece, piece, sems[0].at[k], sems[1].at[k], (me, xp)))
        start(remote(piece, piece, sems[2].at[k], sems[3].at[k], (me, yp)))

    def relay(buf, j, c, near, far):
        s = source(j, c)
        k = j * 2 + c
        piece = buf.at[xp, s]
        remote(piece, piece, near[0].at[k], near[1].at[k], (me, xp)).wait_recv()
        part = buf.at[xp, s, pl.ds(0, half)]
        start(remote(part, part, far[2].at[k], far[3].at[k], (me, yp)))
        piece = buf.at[yp, s]
        remote(piece, piece, near[2].at[k], near[3].at[k], (me, yp)).wait_recv()
        part = buf.at[yp, s, pl.ds(half, experts - half)]
        start(remote(part, part, far[0].at[k], far[1].at[k], (me, xp)))

    def arrive(buf, j, c, far):
        s = source(j, c)
        k = j * 2 + c
        dp = (xp + 2) % 4
        part = buf.at[dp, s, pl.ds(0, half)]
        remote(part, part, far[2].at[k], far[3].at[k], (me, yp)).wait_recv()
        part = buf.at[dp, s, pl.ds(half, experts - half)]
        remote(part, part, far[0].at[k], far[1].at[k], (me, xp)).wait_recv()

    row_near = (x_send, x_recv, y_send, y_recv)
    row_far = (dx_send, dx_recv, dy_send, dy_recv)
    hid_near = (hx_send, hx_recv, hy_send, hy_recv)
    hid_far = (hdx_send, hdx_recv, hdy_send, hdy_recv)

    def stage_a(j):
        if j == 0:
            own.wait()
            other = (core + 1) % 2
            remote(
                rows_ref.at[tp, source(0, other)], rows_ref.at[tp, source(0, other)],
                s_send.at[0], s_recv.at[other], (source(0, other), tp),
            ).wait_recv()
        for c in range(2):
            if j > 0:
                piece = rows_ref.at[tp, source(j, c)]
                remote(
                    piece, piece, s_send.at[0], s_recv.at[j * 2 + c], (source(j, c), tp)
                ).wait_recv()
            exchange(rows_ref, j, c, row_near)

    def stage_b(j):
        for c in range(2):
            relay(rows_ref, j, c, row_near, row_far)

    def stage_c(j):
        if j == 0:
            loads[0].wait()
            loads[1].wait()
        for c in range(2):
            arrive(rows_ref, j, c, row_far)
        first = source(j, 0)

        def one(e, carry):
            gate = jnp.zeros((2 * cap, width), F32)
            up = jnp.zeros((2 * cap, width), F32)
            for q in range(n_tp):
                x = rows_ref[q, pl.ds(first, 2), e].reshape(2 * cap, share)
                cut = slice(q * share, (q + 1) * share)
                gate = gate + jnp.dot(x, gate_ref[e, cut, :], preferred_element_type=F32)
                up = up + jnp.dot(x, up_ref[e, cut, :], preferred_element_type=F32)
            hidden = (silu(gate) * up).astype(BF16)
            hid_ref[tp, pl.ds(first, 2), e] = hidden.reshape(2, cap, width)
            return carry

        lax.fori_loop(0, experts, one, 0)
        for c in range(2):
            exchange(hid_ref, j, c, hid_near)

    def stage_d(j):
        for c in range(2):
            relay(hid_ref, j, c, hid_near, hid_far)

    keep = []

    def stage_e(j):
        if j == 0:
            loads[2].wait()
        for c in range(2):
            arrive(hid_ref, j, c, hid_far)
        first = source(j, 0)

        def one(e, carry):
            total = jnp.zeros((2 * cap, share), F32)
            for q in range(n_tp):
                x = hid_ref[q, pl.ds(first, 2), e].reshape(2 * cap, width)
                cut = slice(q * width, (q + 1) * width)
                total = total + jnp.dot(x, down_ref[e, cut, :], preferred_element_type=F32)
            done_ref[pl.ds(first, 2), e] = total.astype(BF16).reshape(2, cap, share)
            return carry

        lax.fori_loop(0, experts, one, 0)
        if j == 0:
            copy = pltpu.make_async_copy(done_ref.at[me], back_ref.at[me], own_sem.at[1])
            copy.start()
            keep.append(copy)
        for c in range(2):
            if j == 0 and c == 1:
                continue
            target = source(0, (core + 1) % 2) if j == 0 else source(j, c)
            start(
                remote(
                    done_ref.at[target], back_ref.at[me], r_send.at[j * 2 + c],
                    r_recv.at[j * 2 + core], (target, tp),
                )
            )

    stages = (stage_a, stage_b, stage_c, stage_d, stage_e)
    lag = (0, 1, 2, 3, 4)
    for turn in range(planes + lag[-1]):
        for stage, late in zip(stages, lag):
            if 0 <= turn - late < planes:
                stage(turn - late)

    keep[0].wait()
    for j in range(planes):
        for c in range(2):
            if j == 0:
                if c == 1:
                    continue
                other = (core + 1) % 2
                origin, k = source(0, other), other
            else:
                origin, k = ((plane - j + planes) % planes) * 2 + c, j * 2 + c
            piece = back_ref.at[origin]
            remote(piece, piece, r_send.at[0], r_recv.at[k], (origin, tp)).wait_recv()
    for copy in sends:
        copy.wait_send()


def run_experts_plain(slots, expert_gate, expert_up, expert_down):
    experts, _, width = expert_gate.shape
    arrived = lax.all_to_all(slots, "sp", split_axis=0, concat_axis=0, tiled=True)
    rows = lax.all_gather(arrived, "tp", axis=3, tiled=True)
    gate = jnp.einsum("secd,edf->secf", rows, expert_gate, preferred_element_type=F32)
    up = jnp.einsum("secd,edf->secf", rows, expert_up, preferred_element_type=F32)
    hidden = lax.all_gather((jax.nn.silu(gate) * up).astype(BF16), "tp", axis=3, tiled=True)
    done = jnp.einsum("secf,efd->secd", hidden, expert_down, preferred_element_type=F32)
    return lax.all_to_all(done.astype(BF16), "sp", split_axis=0, concat_axis=0, tiled=True)


def run_experts(slots, expert_gate, expert_up, expert_down):
    n_sp, n_tp = lax.axis_size("sp"), lax.axis_size("tp")
    experts, full, width = expert_gate.shape
    share = expert_down.shape[2]
    if n_tp != 4 or n_sp % 2 or experts < 2:
        return run_experts_plain(slots, expert_gate, expert_up, expert_down)
    dma = lambda count: pltpu.SemaphoreType.DMA((count,))
    return pl.pallas_call(
        functools.partial(experts_kernel, n_sp, n_tp),
        out_shape=jax.ShapeDtypeStruct((n_sp, experts, CAP, share), BF16),
        in_specs=[VMEM, ANY, ANY, ANY],
        out_specs=VMEM,
        scratch_shapes=[
            pltpu.VMEM(expert_gate.shape, BF16),
            pltpu.VMEM(expert_up.shape, BF16),
            pltpu.VMEM(expert_down.shape, BF16),
            pltpu.VMEM((n_tp, n_sp, experts, CAP, share), BF16),
            pltpu.VMEM((n_tp, n_sp, experts, CAP, width), BF16),
            pltpu.VMEM((n_sp, experts, CAP, share), BF16),
            dma(3),
            dma(2),
        ]
        + [dma(n_sp) for _ in range(20)],
        compiler_params=pltpu.CompilerParams(
            collective_id=0, has_side_effects=True, vmem_limit_bytes=60 * 2**20
        ),
        cost_estimate=pl.CostEstimate(
            flops=10**10, bytes_accessed=2 * 10**7, transcendentals=10**6
        ),
    )(slots, expert_gate, expert_up, expert_down)


def per_device(
    stream, inner_act, gate_act, state_write, state_read, step_raw, conv_inner, conv_write, conv_read,
    step_bias, decay_log, inner_gain, out_weight, ffn_gain, expert_ids, expert_weights,
    expert_gate, expert_up, expert_down,
):
    length, inner_width = inner_act.shape
    heads = step_raw.shape[1]
    groups, state_dim = state_write.shape[1:]
    per_group = heads // groups
    head_dim = inner_width // heads
    group_width = per_group * head_dim
    write_width = groups * state_dim
    n_sp = lax.axis_size("sp")
    place = lax.axis_index("sp")
    writes = state_write.reshape(length, write_width)
    reads = state_read.reshape(length, write_width)
    last = jnp.concatenate(
        [inner_act[length - HALO :], writes[length - HALO :], reads[length - HALO :]], axis=1
    )
    halo = lax.ppermute(last, "sp", [(i, i + 1) for i in range(n_sp - 1)])

    step_len = jax.nn.softplus(step_raw.astype(F32) + step_bias[None, :])
    rate = -jnp.exp(decay_log)
    lower = jnp.tril(jnp.ones((length, length), F32))
    cumul = jnp.dot(lower, step_len * rate[None, :], precision=HIGH)
    total = cumul[-1]
    to_end = jnp.exp(total[None, :] - cumul) * step_len
    by_group = lambda a: a.reshape(length, groups, per_group).transpose(1, 0, 2)
    cum_g = by_group(cumul)
    cum_t = cum_g.transpose(0, 2, 1)
    step_t = by_group(step_len).transpose(0, 2, 1)
    end_g = by_group(to_end)

    col = lambda rows, cols: pl.BlockSpec((rows, cols), lambda g: (0, g))
    lead = lambda a: pl.BlockSpec((1,) + a.shape[1:], lambda g: (g, 0, 0))
    taps = conv_inner.shape[0]
    params = pltpu.CompilerParams(vmem_limit_bytes=48 * 2**20)
    xs, bw, cr, state = pl.pallas_call(
        functools.partial(conv_kernel, per_group),
        grid=(groups,),
        out_shape=(
            jax.ShapeDtypeStruct((length, inner_width), BF16),
            jax.ShapeDtypeStruct((length, write_width), BF16),
            jax.ShapeDtypeStruct((length, write_width), BF16),
            jax.ShapeDtypeStruct((groups * group_width, state_dim), BF16),
        ),
        in_specs=[
            col(length, group_width), col(length, state_dim), col(length, state_dim),
            col(HALO, group_width), col(HALO, state_dim), col(HALO, state_dim),
            col(taps, group_width), col(taps, state_dim), col(taps, state_dim), lead(end_g),
        ],
        out_specs=(
            col(length, group_width), col(length, state_dim), col(length, state_dim),
            pl.BlockSpec((group_width, state_dim), lambda g: (g, 0)),
        ),
        scratch_shapes=[pltpu.VMEM((length + HALO, max(group_width, state_dim)), F32)],
        compiler_params=params,
        cost_estimate=pl.CostEstimate(flops=10**9, bytes_accessed=10**7, transcendentals=10**6),
    )(
        inner_act, writes, reads,
        halo[:, :inner_width], halo[:, inner_width : inner_width + write_width],
        halo[:, inner_width + write_width :],
        conv_inner, conv_write.reshape(taps, write_width), conv_read.reshape(taps, write_width), end_g,
    )
    states = lax.all_gather(state, "sp")
    totals = lax.all_gather(total, "sp")

    inside = pl.pallas_call(
        functools.partial(inside_kernel, per_group),
        grid=(groups,),
        out_shape=jax.ShapeDtypeStruct((length, inner_width), F32),
        in_specs=[
            col(length, group_width), col(length, state_dim), col(length, state_dim),
            lead(cum_g), lead(cum_t), lead(step_t),
        ],
        out_specs=col(length, group_width),
        compiler_params=params,
        cost_estimate=pl.CostEstimate(
            flops=4 * 10**9, bytes_accessed=10**7, transcendentals=3 * 10**6
        ),
    )(xs, bw, cr, cum_g, cum_t, step_t)

    order = jnp.arange(n_sp)
    between = ((order[None, :] > order[:, None]) & (order[None, :] < place)).astype(F32)
    left = jnp.exp(jnp.sum(between[:, :, None] * totals[None], axis=1))
    left = jnp.where((order < place)[:, None], left, 0.0)
    left = jnp.repeat(left, head_dim, axis=1)
    arriving = jnp.sum(left[:, :, None] * states.astype(F32), axis=0).astype(BF16)

    mixed_inner = pl.pallas_call(
        functools.partial(outside_kernel, per_group),
        grid=(groups,),
        out_shape=jax.ShapeDtypeStruct((length, inner_width), BF16),
        in_specs=[
            col(length, group_width), col(length, state_dim),
            pl.BlockSpec((group_width, state_dim), lambda g: (g, 0)),
            lead(cum_g), col(length, group_width), col(1, group_width),
        ],
        out_specs=col(length, group_width),
        compiler_params=params,
        cost_estimate=pl.CostEstimate(flops=10**9, bytes_accessed=10**7, transcendentals=10**6),
    )(inside, cr, arriving, cum_g, gate_act, inner_gain[None, :])

    partial_value = jnp.dot(mixed_inner, out_weight, preferred_element_type=F32)
    full_width = partial_value.shape[1]
    local_experts = expert_gate.shape[0]
    expert_count = local_experts * n_sp
    ids = expert_ids.reshape(-1)
    onehot = (ids[:, None] == jnp.arange(expert_count, dtype=jnp.int32)[None, :]).astype(BF16)
    pairs = ids.shape[0]
    before = jnp.tril(jnp.ones((pairs, pairs), BF16), -1)
    earlier = jnp.dot(before, onehot, preferred_element_type=F32)
    slot_of = jnp.sum(earlier * onehot.astype(F32), axis=1).astype(jnp.int32)
    target = (ids * CAP + slot_of).reshape(length, TOPK)
    slots = jnp.arange(expert_count * CAP, dtype=jnp.int32)
    named = [target[:, k][:, None] == slots[None, :] for k in range(TOPK)]
    place_of = functools.reduce(jnp.logical_or, named).astype(BF16)
    mix = functools.reduce(
        jnp.add, [jnp.where(n, expert_weights[:, k : k + 1], 0.0) for k, n in enumerate(named)]
    )
    mix_high = mix.astype(BF16)
    mix_low = (mix - mix_high.astype(F32)).astype(BF16)

    out_width = expert_down.shape[2]
    own_start = lax.axis_index("tp") * out_width
    projected = lax.psum_scatter(
        partial_value.astype(BF16), "tp", scatter_dimension=1, tiled=True
    ).astype(F32)
    kept = lax.dynamic_slice_in_dim(stream, own_start, out_width, 1).astype(F32) + projected
    square_total = lax.psum(jnp.sum(kept * kept, axis=1), "tp")
    gain_share = lax.dynamic_slice_in_dim(ffn_gain, own_start, out_width, 0)
    scale_rows = lax.rsqrt(square_total / full_width + EPS)
    normed = (kept * scale_rows[:, None] * gain_share[None, :]).astype(BF16)
    outgoing = tn_dot(place_of, normed).astype(BF16)
    back = run_experts(
        outgoing.reshape(n_sp, local_experts, CAP, out_width), expert_gate, expert_up, expert_down
    )
    results = back.reshape(expert_count * CAP, out_width)
    moe = jnp.dot(mix_high, results, preferred_element_type=F32) + jnp.dot(
        mix_low, results, preferred_element_type=F32
    )
    return (kept + moe).astype(BF16)


def solution(mesh):
    return jax.shard_map(
        per_device,
        mesh=mesh,
        in_specs=(
            P("sp", None), P("sp", "tp"), P("sp", "tp"), P("sp", "tp", None), P("sp", "tp", None),
            P("sp", "tp"), P(None, "tp"), P(None, "tp", None), P(None, "tp", None), P("tp"), P("tp"),
            P("tp"), P("tp", None), P(), P("sp", None), P("sp", None), P("sp", None, "tp"),
            P("sp", None, "tp"), P("sp", None, "tp"),
        ),
        out_specs=P("sp", "tp"),
        check_vma=False,
    )
```

```python
import functools

import jax
import jax.numpy as jnp
from jax import lax
from jax.experimental import pallas as pl
from jax.experimental.pallas import tpu as pltpu
from jax.sharding import PartitionSpec as P

TOPK = 2
CAP = 48
EPS = 1e-06
HIGH = lax.Precision.HIGHEST
MESH = pl.DeviceIdType.MESH
HALO = 8
VMEM = pl.BlockSpec(memory_space=pltpu.VMEM)
ANY = pl.BlockSpec(memory_space=pl.ANY)
F32 = jnp.float32
BF16 = jnp.bfloat16


def silu(x):
    return x / (1.0 + jnp.exp(-x))


def nt_dot(a, b):
    return lax.dot_general(a, b, (((1,), (1,)), ((), ())), preferred_element_type=F32)


def tn_dot(a, b):
    return lax.dot_general(a, b, (((0,), (0,)), ((), ())), preferred_element_type=F32)


def conv_kernel(
    per_group, x_ref, w_ref, r_ref, hx_ref, hw_ref, hr_ref, kx_ref, kw_ref, kr_ref, end_ref, sum_ref,
    xs_ref, bw_ref, cr_ref, state_ref, pad_ref,
):
    length = x_ref.shape[0]

    def conv(src_ref, halo_ref, tap_ref):
        width = src_ref.shape[1]
        pad_ref[0:HALO, 0:width] = halo_ref[...].astype(F32)
        pad_ref[HALO : HALO + length, 0:width] = src_ref[...].astype(F32)
        taps = tap_ref[...].astype(F32)
        count = taps.shape[0]
        total = jnp.zeros((length, width), F32)
        for k in range(count):
            begin = HALO + k - count + 1
            total = total + taps[k : k + 1, :] * pad_ref[begin : begin + length, 0:width]
        return silu(total)

    xs = conv(x_ref, hx_ref, kx_ref)
    bw = conv(w_ref, hw_ref, kw_ref).astype(BF16)
    cr_ref[...] = conv(r_ref, hr_ref, kr_ref).astype(BF16)
    xs_ref[...] = xs.astype(BF16)
    bw_ref[...] = bw
    head_dim = xs.shape[1] // per_group
    scaled = [
        xs[:, h * head_dim : (h + 1) * head_dim] * end_ref[0, :, h : h + 1] for h in range(per_group)
    ]
    weighted = jnp.concatenate(scaled, axis=1).astype(BF16)
    state_ref[0, 0 : xs.shape[1], :] = tn_dot(weighted, bw).astype(BF16)
    terms = []
    rest = [jnp.broadcast_to(sum_ref[0, :, h : h + 1], (1, bw.shape[1])) for h in range(per_group)]
    for _ in range(3):
        cut = [r.astype(BF16).astype(F32) for r in rest]
        terms += cut
        rest = [r - c for r, c in zip(rest, cut)]
    blank = jnp.zeros((state_ref.shape[1] - xs.shape[1] - len(terms), bw.shape[1]), F32)
    state_ref[0, xs.shape[1] :, :] = jnp.concatenate(terms + [blank], axis=0).astype(BF16)


def inside_kernel(per_group, xs_ref, bw_ref, cr_ref, cum_ref, cumt_ref, stept_ref, out_ref):
    length = xs_ref.shape[0]
    head_dim = xs_ref.shape[1] // per_group
    scores = nt_dot(cr_ref[...], bw_ref[...])
    rows = lax.broadcasted_iota(jnp.int32, (length, length), 0)
    columns = lax.broadcasted_iota(jnp.int32, (length, length), 1)
    causal = rows >= columns
    pieces = []
    for h in range(per_group):
        spread = cum_ref[0, :, h : h + 1] - cumt_ref[0, h : h + 1, :]
        within = jnp.exp(jnp.where(causal, spread, -1e30))
        mixing = (scores * within * stept_ref[0, h : h + 1, :]).astype(BF16)
        pieces.append(
            jnp.dot(
                mixing, xs_ref[:, h * head_dim : (h + 1) * head_dim], preferred_element_type=F32
            )
        )
    out_ref[...] = jnp.concatenate(pieces, axis=1)


def outside_kernel(
    per_group, in_ref, cr_ref, state_ref, cum_ref, gate_ref, gain_ref, out_ref
):
    head_dim = in_ref.shape[1] // per_group
    width = in_ref.shape[1]
    place = lax.axis_index("sp")
    entering = []
    for h in range(per_group):
        cut = slice(h * head_dim, (h + 1) * head_dim)
        held = jnp.zeros((head_dim, state_ref.shape[3]), F32)
        for j in range(state_ref.shape[0]):
            tail = state_ref[j, 0, width:, :].astype(F32)
            total = sum(tail[i * per_group + h : i * per_group + h + 1, :] for i in range(3))
            later = held * jnp.exp(total) + state_ref[j, 0, cut, :].astype(F32)
            held = jnp.where(j < place, later, held)
        entering.append(held)
    arriving = jnp.concatenate(entering, axis=0).astype(BF16)
    outside = nt_dot(cr_ref[...], arriving)
    gates = silu(gate_ref[...].astype(F32))
    pieces = []
    for h in range(per_group):
        cut = slice(h * head_dim, (h + 1) * head_dim)
        part = in_ref[:, cut] + outside[:, cut] * jnp.exp(cum_ref[0, :, h : h + 1])
        part = part * gates[:, cut]
        scale = lax.rsqrt(jnp.mean(part * part, axis=1, keepdims=True) + EPS)
        pieces.append(part * scale)
    out_ref[...] = (jnp.concatenate(pieces, axis=1) * gain_ref[...]).astype(BF16)


def project_kernel(
    mixed_ref, weight_ref, stream_ref, gain_ref, place_ref, kept_ref, slots_ref,
    part_ref, got_ref, hop_ref, square_ref, squares_ref,
    n_send, n_recv, h_send, h_recv, f_send, f_recv, q_send, q_recv,
):
    me = lax.axis_index("sp")
    tp = lax.axis_index("tp")
    xp = tp + 1 - 2 * (tp % 2)
    yp = (tp + 2) % 4
    dp = (xp + 2) % 4
    length, share = kept_ref.shape
    half = length // 2

    barrier = pltpu.get_barrier_semaphore()
    for peer in (xp, yp, dp):
        pl.semaphore_signal(barrier, inc=1, device_id=(me, peer), device_id_type=MESH)
    pl.semaphore_wait(barrier, 3)

    def remote(src, dst, send, recv, peer):
        return pltpu.make_async_remote_copy(
            src_ref=src, dst_ref=dst, send_sem=send, recv_sem=recv,
            device_id=(me, peer), device_id_type=MESH,
        )

    def term(q):
        columns = pl.ds(pl.multiple_of(q * share, share), share)
        return jnp.dot(mixed_ref[...], weight_ref[:, columns], preferred_element_type=F32).astype(BF16)

    part_ref[2] = term(dp)
    first, second = pl.ds(0, half), pl.ds(half, half)
    hops = [
        remote(part_ref.at[2, first], hop_ref.at[0], h_send.at[0], h_recv.at[0], xp),
        remote(part_ref.at[2, second], hop_ref.at[1], h_send.at[1], h_recv.at[1], yp),
    ]
    for copy in hops:
        copy.start()
    near = []
    for i, peer in enumerate((xp, yp)):
        part_ref[i] = term(peer)
        copy = remote(part_ref.at[i], got_ref.at[i], n_send.at[i], n_recv.at[i], peer)
        copy.start()
        near.append(copy)
    kept = stream_ref[...].astype(F32) + term(tp).astype(F32)
    passed = [
        remote(hop_ref.at[0], got_ref.at[2, first], f_send.at[0], f_recv.at[0], yp),
        remote(hop_ref.at[1], got_ref.at[2, second], f_send.at[1], f_recv.at[1], xp),
    ]
    for hop, copy in zip(hops, passed):
        hop.wait_recv()
        copy.start()
    for copy in near + passed:
        copy.wait_recv()
    for i in range(3):
        kept = kept + got_ref[i].astype(F32)
    kept_ref[...] = kept
    ones = jnp.ones((8, share), F32)
    square_ref[...] = lax.dot_general(
        ones, kept * kept, (((1,), (1,)), ((), ())), precision=HIGH, preferred_element_type=F32
    )
    asks = []
    for i, peer in enumerate((xp, yp, dp)):
        copy = remote(square_ref, squares_ref.at[i], q_send.at[i], q_recv.at[i], peer)
        copy.start()
        asks.append(copy)
    for copy in asks:
        copy.wait_recv()
    squares = square_ref[...] + squares_ref[0] + squares_ref[1] + squares_ref[2]
    scale = lax.rsqrt(squares / weight_ref.shape[1] + EPS)
    pick = jnp.full((8, share), 0.125, F32)
    spread = lax.dot_general(
        scale, pick, (((0,), (0,)), ((), ())), precision=HIGH, preferred_element_type=F32
    )
    normed = (kept * spread * gain_ref[...]).astype(BF16)
    for i in range(slots_ref.shape[0]):
        slots_ref[i] = jnp.dot(place_ref[i], normed, preferred_element_type=F32).astype(BF16)
    for copy in hops + near + passed + asks:
        copy.wait_send()


def run_project(mixed, weight, stream_share, gain_share, place_of):
    n_tp = lax.axis_size("tp")
    length, share = stream_share.shape
    if n_tp != 4 or length % 32:
        partial_value = jnp.dot(mixed, weight, preferred_element_type=F32).astype(BF16)
        projected = lax.psum_scatter(partial_value, "tp", scatter_dimension=1, tiled=True)
        kept = stream_share.astype(F32) + projected.astype(F32)
        squares = lax.psum(jnp.sum(kept * kept, axis=1), "tp")
        scale = lax.rsqrt(squares / weight.shape[1] + EPS)
        normed = (kept * scale[:, None] * gain_share[None, :]).astype(BF16)
        slots = jnp.einsum("ist,td->isd", place_of, normed, preferred_element_type=F32)
        return kept, slots.astype(BF16)
    dma = lambda count: pltpu.SemaphoreType.DMA((count,))
    return pl.pallas_call(
        project_kernel,
        out_shape=(
            jax.ShapeDtypeStruct((length, share), F32),
            jax.ShapeDtypeStruct(place_of.shape[:2] + (share,), BF16),
        ),
        in_specs=[VMEM] * 5,
        out_specs=(VMEM, VMEM),
        scratch_shapes=[
            pltpu.VMEM((3, length, share), BF16),
            pltpu.VMEM((3, length, share), BF16),
            pltpu.VMEM((2, length // 2, share), BF16),
            pltpu.VMEM((8, length), F32),
            pltpu.VMEM((3, 8, length), F32),
            dma(2), dma(2), dma(2), dma(2), dma(2), dma(2), dma(3), dma(3),
        ],
        compiler_params=pltpu.CompilerParams(
            collective_id=1, has_side_effects=True, vmem_limit_bytes=48 * 2**20
        ),
        cost_estimate=pl.CostEstimate(
            flops=4 * 10**9, bytes_accessed=10**7, transcendentals=10**4
        ),
    )(mixed, weight, stream_share, gain_share[None, :], place_of)


def experts_kernel(
    n_sp, n_tp, slots_ref, gate_hbm, up_hbm, down_hbm, back_ref,
    gate_ref, up_ref, down_ref, rows_ref, hid_ref, done_ref,
    w_sem, own_sem, s_send, s_recv, x_send, x_recv, y_send, y_recv, dx_send, dx_recv, dy_send, dy_recv,
    hx_send, hx_recv, hy_send, hy_recv, hdx_send, hdx_recv, hdy_send, hdy_recv, r_send, r_recv,
):
    me = lax.axis_index("sp")
    tp = lax.axis_index("tp")
    plane, core = me // 2, me % 2
    planes = n_sp // 2
    xp = tp + 1 - 2 * (tp % 2)
    yp = (tp + 2) % 4
    experts = gate_ref.shape[0]
    half = experts // 2
    cap = rows_ref.shape[3]
    share = rows_ref.shape[4]
    width = hid_ref.shape[4]

    barrier = pltpu.get_barrier_semaphore()
    for step in range(1, n_sp):
        pl.semaphore_signal(
            barrier, inc=1, device_id=((me + step) % n_sp, tp), device_id_type=MESH
        )
    for peer in (xp, yp):
        pl.semaphore_signal(barrier, inc=1, device_id=(me, peer), device_id_type=MESH)
    pl.semaphore_wait(barrier, n_sp + 1)

    sends = []

    def remote(src, dst, send, recv, device):
        return pltpu.make_async_remote_copy(
            src_ref=src, dst_ref=dst, send_sem=send, recv_sem=recv,
            device_id=device, device_id_type=MESH,
        )

    def start(copy):
        copy.start()
        sends.append(copy)

    own = pltpu.make_async_copy(slots_ref.at[me], rows_ref.at[tp, me], own_sem.at[0])
    own.start()
    for j in range(planes):
        for c in range(2):
            if j == 0 and c == 1:
                continue
            to_core = (core + 1) % 2 if j == 0 else c
            target = ((plane - j + planes) % planes) * 2 + to_core
            start(
                remote(
                    slots_ref.at[target], rows_ref.at[tp, me], s_send.at[j * 2 + c],
                    s_recv.at[j * 2 + core], (target, tp),
                )
            )
    loads = [
        pltpu.make_async_copy(a, b, w_sem.at[i])
        for i, (a, b) in enumerate(
            ((gate_hbm, gate_ref), (up_hbm, up_ref), (down_hbm, down_ref))
        )
    ]
    for load in loads:
        load.start()

    def source(j, c):
        return ((plane + j) % planes) * 2 + c

    def exchange(buf, j, c, sems):
        s = source(j, c)
        k = j * 2 + c
        piece = buf.at[tp, s]
        start(remote(piece, piece, sems[0].at[k], sems[1].at[k], (me, xp)))
        start(remote(piece, piece, sems[2].at[k], sems[3].at[k], (me, yp)))

    def relay(buf, j, c, near, far):
        s = source(j, c)
        k = j * 2 + c
        piece = buf.at[xp, s]
        remote(piece, piece, near[0].at[k], near[1].at[k], (me, xp)).wait_recv()
        part = buf.at[xp, s, pl.ds(0, half)]
        start(remote(part, part, far[2].at[k], far[3].at[k], (me, yp)))
        piece = buf.at[yp, s]
        remote(piece, piece, near[2].at[k], near[3].at[k], (me, yp)).wait_recv()
        part = buf.at[yp, s, pl.ds(half, experts - half)]
        start(remote(part, part, far[0].at[k], far[1].at[k], (me, xp)))

    def arrive(buf, j, c, far):
        s = source(j, c)
        k = j * 2 + c
        dp = (xp + 2) % 4
        part = buf.at[dp, s, pl.ds(0, half)]
        remote(part, part, far[2].at[k], far[3].at[k], (me, yp)).wait_recv()
        part = buf.at[dp, s, pl.ds(half, experts - half)]
        remote(part, part, far[0].at[k], far[1].at[k], (me, xp)).wait_recv()

    row_near = (x_send, x_recv, y_send, y_recv)
    row_far = (dx_send, dx_recv, dy_send, dy_recv)
    hid_near = (hx_send, hx_recv, hy_send, hy_recv)
    hid_far = (hdx_send, hdx_recv, hdy_send, hdy_recv)

    def stage_a(j):
        if j == 0:
            own.wait()
            other = (core + 1) % 2
            remote(
                rows_ref.at[tp, source(0, other)], rows_ref.at[tp, source(0, other)],
                s_send.at[0], s_recv.at[other], (source(0, other), tp),
            ).wait_recv()
        for c in range(2):
            if j > 0:
                piece = rows_ref.at[tp, source(j, c)]
                remote(
                    piece, piece, s_send.at[0], s_recv.at[j * 2 + c], (source(j, c), tp)
                ).wait_recv()
            exchange(rows_ref, j, c, row_near)

    def stage_b(j):
        for c in range(2):
            relay(rows_ref, j, c, row_near, row_far)

    def stage_c(j):
        if j == 0:
            loads[0].wait()
            loads[1].wait()
        for c in range(2):
            arrive(rows_ref, j, c, row_far)
        first = source(j, 0)

        def one(e, carry):
            gate = jnp.zeros((2 * cap, width), F32)
            up = jnp.zeros((2 * cap, width), F32)
            for q in range(n_tp):
                x = rows_ref[q, pl.ds(first, 2), e].reshape(2 * cap, share)
                cut = slice(q * share, (q + 1) * share)
                gate = gate + jnp.dot(x, gate_ref[e, cut, :], preferred_element_type=F32)
                up = up + jnp.dot(x, up_ref[e, cut, :], preferred_element_type=F32)
            hidden = (silu(gate) * up).astype(BF16)
            hid_ref[tp, pl.ds(first, 2), e] = hidden.reshape(2, cap, width)
            return carry

        lax.fori_loop(0, experts, one, 0)
        for c in range(2):
            exchange(hid_ref, j, c, hid_near)

    def stage_d(j):
        for c in range(2):
            relay(hid_ref, j, c, hid_near, hid_far)

    keep = []

    def stage_e(j):
        if j == 0:
            loads[2].wait()
        for c in range(2):
            arrive(hid_ref, j, c, hid_far)
        first = source(j, 0)

        def one(e, carry):
            total = jnp.zeros((2 * cap, share), F32)
            for q in range(n_tp):
                x = hid_ref[q, pl.ds(first, 2), e].reshape(2 * cap, width)
                cut = slice(q * width, (q + 1) * width)
                total = total + jnp.dot(x, down_ref[e, cut, :], preferred_element_type=F32)
            done_ref[pl.ds(first, 2), e] = total.astype(BF16).reshape(2, cap, share)
            return carry

        lax.fori_loop(0, experts, one, 0)
        if j == 0:
            copy = pltpu.make_async_copy(done_ref.at[me], back_ref.at[me], own_sem.at[1])
            copy.start()
            keep.append(copy)
        for c in range(2):
            if j == 0 and c == 1:
                continue
            target = source(0, (core + 1) % 2) if j == 0 else source(j, c)
            start(
                remote(
                    done_ref.at[target], back_ref.at[me], r_send.at[j * 2 + c],
                    r_recv.at[j * 2 + core], (target, tp),
                )
            )

    stages = (stage_a, stage_b, stage_c, stage_d, stage_e)
    lag = (0, 1, 2, 3, 4)
    for turn in range(planes + lag[-1]):
        for stage, late in zip(stages, lag):
            if 0 <= turn - late < planes:
                stage(turn - late)

    keep[0].wait()
    for j in range(planes):
        for c in range(2):
            if j == 0:
                if c == 1:
                    continue
                other = (core + 1) % 2
                origin, k = source(0, other), other
            else:
                origin, k = ((plane - j + planes) % planes) * 2 + c, j * 2 + c
            piece = back_ref.at[origin]
            remote(piece, piece, r_send.at[0], r_recv.at[k], (origin, tp)).wait_recv()
    for copy in sends:
        copy.wait_send()


def run_experts_plain(slots, expert_gate, expert_up, expert_down):
    experts, _, width = expert_gate.shape
    arrived = lax.all_to_all(slots, "sp", split_axis=0, concat_axis=0, tiled=True)
    rows = lax.all_gather(arrived, "tp", axis=3, tiled=True)
    gate = jnp.einsum("secd,edf->secf", rows, expert_gate, preferred_element_type=F32)
    up = jnp.einsum("secd,edf->secf", rows, expert_up, preferred_element_type=F32)
    hidden = lax.all_gather((jax.nn.silu(gate) * up).astype(BF16), "tp", axis=3, tiled=True)
    done = jnp.einsum("secf,efd->secd", hidden, expert_down, preferred_element_type=F32)
    return lax.all_to_all(done.astype(BF16), "sp", split_axis=0, concat_axis=0, tiled=True)


def run_experts(slots, expert_gate, expert_up, expert_down):
    n_sp, n_tp = lax.axis_size("sp"), lax.axis_size("tp")
    experts, full, width = expert_gate.shape
    share = expert_down.shape[2]
    if n_tp != 4 or n_sp % 2 or experts < 2:
        return run_experts_plain(slots, expert_gate, expert_up, expert_down)
    dma = lambda count: pltpu.SemaphoreType.DMA((count,))
    return pl.pallas_call(
        functools.partial(experts_kernel, n_sp, n_tp),
        out_shape=jax.ShapeDtypeStruct((n_sp, experts, CAP, share), BF16),
        in_specs=[VMEM, ANY, ANY, ANY],
        out_specs=VMEM,
        scratch_shapes=[
            pltpu.VMEM(expert_gate.shape, BF16),
            pltpu.VMEM(expert_up.shape, BF16),
            pltpu.VMEM(expert_down.shape, BF16),
            pltpu.VMEM((n_tp, n_sp, experts, CAP, share), BF16),
            pltpu.VMEM((n_tp, n_sp, experts, CAP, width), BF16),
            pltpu.VMEM((n_sp, experts, CAP, share), BF16),
            dma(3),
            dma(2),
        ]
        + [dma(n_sp) for _ in range(20)],
        compiler_params=pltpu.CompilerParams(
            collective_id=0, has_side_effects=True, vmem_limit_bytes=60 * 2**20
        ),
        cost_estimate=pl.CostEstimate(
            flops=10**10, bytes_accessed=2 * 10**7, transcendentals=10**6
        ),
    )(slots, expert_gate, expert_up, expert_down)


def per_device(
    stream, inner_act, gate_act, state_write, state_read, step_raw, conv_inner, conv_write, conv_read,
    step_bias, decay_log, inner_gain, out_weight, ffn_gain, expert_ids, expert_weights,
    expert_gate, expert_up, expert_down,
):
    length, inner_width = inner_act.shape
    heads = step_raw.shape[1]
    groups, state_dim = state_write.shape[1:]
    per_group = heads // groups
    head_dim = inner_width // heads
    group_width = per_group * head_dim
    write_width = groups * state_dim
    n_sp = lax.axis_size("sp")
    writes = state_write.reshape(length, write_width)
    reads = state_read.reshape(length, write_width)
    last = jnp.concatenate(
        [inner_act[length - HALO :], writes[length - HALO :], reads[length - HALO :]], axis=1
    )
    halo = lax.ppermute(last, "sp", [(i, i + 1) for i in range(n_sp - 1)])

    step_len = jax.nn.softplus(step_raw.astype(F32) + step_bias[None, :])
    rate = -jnp.exp(decay_log)
    lower = jnp.tril(jnp.ones((length, length), F32))
    cumul = jnp.dot(lower, step_len * rate[None, :], precision=HIGH)
    total = cumul[-1]
    to_end = jnp.exp(total[None, :] - cumul) * step_len
    by_group = lambda a: a.reshape(length, groups, per_group).transpose(1, 0, 2)
    cum_g = by_group(cumul)
    cum_t = cum_g.transpose(0, 2, 1)
    step_t = by_group(step_len).transpose(0, 2, 1)
    end_g = by_group(to_end)
    sum_g = total.reshape(groups, 1, per_group)
    state_rows = group_width + -(-3 * per_group // 16) * 16

    col = lambda rows, cols: pl.BlockSpec((rows, cols), lambda g: (0, g))
    lead = lambda a: pl.BlockSpec((1,) + a.shape[1:], lambda g: (g, 0, 0))
    taps = conv_inner.shape[0]
    params = pltpu.CompilerParams(vmem_limit_bytes=48 * 2**20)
    xs, bw, cr, state = pl.pallas_call(
        functools.partial(conv_kernel, per_group),
        grid=(groups,),
        out_shape=(
            jax.ShapeDtypeStruct((length, inner_width), BF16),
            jax.ShapeDtypeStruct((length, write_width), BF16),
            jax.ShapeDtypeStruct((length, write_width), BF16),
            jax.ShapeDtypeStruct((groups, state_rows, state_dim), BF16),
        ),
        in_specs=[
            col(length, group_width), col(length, state_dim), col(length, state_dim),
            col(HALO, group_width), col(HALO, state_dim), col(HALO, state_dim),
            col(taps, group_width), col(taps, state_dim), col(taps, state_dim), lead(end_g),
            lead(sum_g),
        ],
        out_specs=(
            col(length, group_width), col(length, state_dim), col(length, state_dim),
            pl.BlockSpec((1, state_rows, state_dim), lambda g: (g, 0, 0)),
        ),
        scratch_shapes=[pltpu.VMEM((length + HALO, max(group_width, state_dim)), F32)],
        compiler_params=params,
        cost_estimate=pl.CostEstimate(flops=10**9, bytes_accessed=10**7, transcendentals=10**6),
    )(
        inner_act, writes, reads,
        halo[:, :inner_width], halo[:, inner_width : inner_width + write_width],
        halo[:, inner_width + write_width :],
        conv_inner, conv_write.reshape(taps, write_width), conv_read.reshape(taps, write_width), end_g, sum_g,
    )
    states = lax.all_gather(state, "sp")

    inside = pl.pallas_call(
        functools.partial(inside_kernel, per_group),
        grid=(groups,),
        out_shape=jax.ShapeDtypeStruct((length, inner_width), F32),
        in_specs=[
            col(length, group_width), col(length, state_dim), col(length, state_dim),
            lead(cum_g), lead(cum_t), lead(step_t),
        ],
        out_specs=col(length, group_width),
        compiler_params=params,
        cost_estimate=pl.CostEstimate(
            flops=4 * 10**9, bytes_accessed=10**7, transcendentals=3 * 10**6
        ),
    )(xs, bw, cr, cum_g, cum_t, step_t)

    mixed_inner = pl.pallas_call(
        functools.partial(outside_kernel, per_group),
        grid=(groups,),
        out_shape=jax.ShapeDtypeStruct((length, inner_width), BF16),
        in_specs=[
            col(length, group_width), col(length, state_dim),
            pl.BlockSpec((n_sp, 1, state_rows, state_dim), lambda g: (0, g, 0, 0)),
            lead(cum_g), col(length, group_width), col(1, group_width),
        ],
        out_specs=col(length, group_width),
        compiler_params=params,
        cost_estimate=pl.CostEstimate(flops=10**9, bytes_accessed=10**7, transcendentals=10**6),
    )(inside, cr, states, cum_g, gate_act, inner_gain[None, :])

    local_experts = expert_gate.shape[0]
    expert_count = local_experts * n_sp
    ids = expert_ids.reshape(-1)
    onehot = (ids[:, None] == jnp.arange(expert_count, dtype=jnp.int32)[None, :]).astype(BF16)
    pairs = ids.shape[0]
    before = jnp.tril(jnp.ones((pairs, pairs), BF16), -1)
    earlier = jnp.dot(before, onehot, preferred_element_type=F32)
    slot_of = jnp.sum(earlier * onehot.astype(F32), axis=1).astype(jnp.int32)
    target = (ids * CAP + slot_of).reshape(length, TOPK)
    slots = jnp.arange(expert_count * CAP, dtype=jnp.int32)
    named = [target[:, k][:, None] == slots[None, :] for k in range(TOPK)]
    placed = [slots[:, None] == target[:, k][None, :] for k in range(TOPK)]
    place_of = functools.reduce(jnp.logical_or, placed).astype(BF16)
    mix = functools.reduce(
        jnp.add, [jnp.where(n, expert_weights[:, k : k + 1], 0.0) for k, n in enumerate(named)]
    )
    mix_high = mix.astype(BF16)
    mix_low = (mix - mix_high.astype(F32)).astype(BF16)

    out_width = expert_down.shape[2]
    own_start = lax.axis_index("tp") * out_width
    stream_share = lax.dynamic_slice_in_dim(stream, own_start, out_width, 1)
    gain_share = lax.dynamic_slice_in_dim(ffn_gain, own_start, out_width, 0)
    kept, outgoing = run_project(
        mixed_inner, out_weight, stream_share, gain_share, place_of.reshape(n_sp, -1, length)
    )
    back = run_experts(
        outgoing.reshape(n_sp, local_experts, CAP, out_width), expert_gate, expert_up, expert_down
    )
    results = back.reshape(expert_count * CAP, out_width)
    moe = jnp.dot(mix_high, results, preferred_element_type=F32) + jnp.dot(
        mix_low, results, preferred_element_type=F32
    )
    return (kept + moe).astype(BF16)


def solution(mesh):
    return jax.shard_map(
        per_device,
        mesh=mesh,
        in_specs=(
            P("sp", None), P("sp", "tp"), P("sp", "tp"), P("sp", "tp", None), P("sp", "tp", None),
            P("sp", "tp"), P(None, "tp"), P(None, "tp", None), P(None, "tp", None), P("tp"), P("tp"),
            P("tp"), P("tp", None), P(), P("sp", None), P("sp", None), P("sp", None, "tp"),
            P("sp", None, "tp"), P("sp", None, "tp"),
        ),
        out_specs=P("sp", "tp"),
        check_vma=False,
    )
```

```python
import functools

import jax
import jax.numpy as jnp
from jax import lax
from jax.experimental import pallas as pl
from jax.experimental.pallas import tpu as pltpu
from jax.sharding import PartitionSpec as P

TOPK = 2
CAP = 48
EPS = 1e-06
HIGH = lax.Precision.HIGHEST
MESH = pl.DeviceIdType.MESH
HALO = 8
VMEM = pl.BlockSpec(memory_space=pltpu.VMEM)
ANY = pl.BlockSpec(memory_space=pl.ANY)
F32 = jnp.float32
BF16 = jnp.bfloat16


def silu(x):
    return x / (1.0 + jnp.exp(-x))


def nt_dot(a, b):
    return lax.dot_general(a, b, (((1,), (1,)), ((), ())), preferred_element_type=F32)


def tn_dot(a, b):
    return lax.dot_general(a, b, (((0,), (0,)), ((), ())), preferred_element_type=F32)


def conv_kernel(
    per_group, x_ref, w_ref, r_ref, hx_ref, hw_ref, hr_ref, kx_ref, kw_ref, kr_ref, end_ref, sum_ref,
    xs_ref, bw_ref, cr_ref, state_ref, pad_ref,
):
    length = x_ref.shape[0]

    def conv(src_ref, halo_ref, tap_ref):
        width = src_ref.shape[1]
        pad_ref[0:HALO, 0:width] = halo_ref[...].astype(F32)
        pad_ref[HALO : HALO + length, 0:width] = src_ref[...].astype(F32)
        taps = tap_ref[...].astype(F32)
        count = taps.shape[0]
        total = jnp.zeros((length, width), F32)
        for k in range(count):
            begin = HALO + k - count + 1
            total = total + taps[k : k + 1, :] * pad_ref[begin : begin + length, 0:width]
        return silu(total)

    xs = conv(x_ref, hx_ref, kx_ref)
    bw = conv(w_ref, hw_ref, kw_ref).astype(BF16)
    cr_ref[...] = conv(r_ref, hr_ref, kr_ref).astype(BF16)
    xs_ref[...] = xs.astype(BF16)
    bw_ref[...] = bw
    head_dim = xs.shape[1] // per_group
    scaled = [
        xs[:, h * head_dim : (h + 1) * head_dim] * end_ref[0, :, h : h + 1] for h in range(per_group)
    ]
    weighted = jnp.concatenate(scaled, axis=1).astype(BF16)
    state_ref[0, 0 : xs.shape[1], :] = tn_dot(weighted, bw).astype(BF16)
    terms = []
    rest = [jnp.broadcast_to(sum_ref[0, :, h : h + 1], (1, bw.shape[1])) for h in range(per_group)]
    for _ in range(3):
        cut = [r.astype(BF16).astype(F32) for r in rest]
        terms += cut
        rest = [r - c for r, c in zip(rest, cut)]
    blank = jnp.zeros((state_ref.shape[1] - xs.shape[1] - len(terms), bw.shape[1]), F32)
    state_ref[0, xs.shape[1] :, :] = jnp.concatenate(terms + [blank], axis=0).astype(BF16)


def inside_kernel(per_group, xs_ref, bw_ref, cr_ref, cum_ref, cumt_ref, stept_ref, out_ref):
    length = xs_ref.shape[0]
    head_dim = xs_ref.shape[1] // per_group
    scores = nt_dot(cr_ref[...], bw_ref[...])
    rows = lax.broadcasted_iota(jnp.int32, (length, length), 0)
    columns = lax.broadcasted_iota(jnp.int32, (length, length), 1)
    causal = rows >= columns
    pieces = []
    for h in range(per_group):
        spread = cum_ref[0, :, h : h + 1] - cumt_ref[0, h : h + 1, :]
        within = jnp.exp(jnp.where(causal, spread, -1e30))
        mixing = (scores * within * stept_ref[0, h : h + 1, :]).astype(BF16)
        pieces.append(
            jnp.dot(
                mixing, xs_ref[:, h * head_dim : (h + 1) * head_dim], preferred_element_type=F32
            )
        )
    out_ref[...] = jnp.concatenate(pieces, axis=1)


def outside_kernel(
    per_group, in_ref, cr_ref, state_ref, cum_ref, gate_ref, gain_ref, out_ref
):
    head_dim = in_ref.shape[1] // per_group
    width = in_ref.shape[1]
    place = lax.axis_index("sp")
    entering = []
    for h in range(per_group):
        cut = slice(h * head_dim, (h + 1) * head_dim)
        held = jnp.zeros((head_dim, state_ref.shape[3]), F32)
        for j in range(state_ref.shape[0]):
            tail = state_ref[j, 0, width:, :].astype(F32)
            total = sum(tail[i * per_group + h : i * per_group + h + 1, :] for i in range(3))
            later = held * jnp.exp(total) + state_ref[j, 0, cut, :].astype(F32)
            held = jnp.where(j < place, later, held)
        entering.append(held)
    arriving = jnp.concatenate(entering, axis=0).astype(BF16)
    outside = nt_dot(cr_ref[...], arriving)
    gates = silu(gate_ref[...].astype(F32))
    pieces = []
    for h in range(per_group):
        cut = slice(h * head_dim, (h + 1) * head_dim)
        part = in_ref[:, cut] + outside[:, cut] * jnp.exp(cum_ref[0, :, h : h + 1])
        part = part * gates[:, cut]
        scale = lax.rsqrt(jnp.mean(part * part, axis=1, keepdims=True) + EPS)
        pieces.append(part * scale)
    out_ref[...] = (jnp.concatenate(pieces, axis=1) * gain_ref[...]).astype(BF16)


def project_kernel(
    mixed_ref, weight_ref, stream_ref, gain_ref, place_ref, kept_ref, slots_ref,
    part_ref, got_ref, hop_ref, square_ref, squares_ref,
    n_send, n_recv, h_send, h_recv, f_send, f_recv, q_send, q_recv,
):
    me = lax.axis_index("sp")
    tp = lax.axis_index("tp")
    xp = tp + 1 - 2 * (tp % 2)
    yp = (tp + 2) % 4
    dp = (xp + 2) % 4
    length, share = kept_ref.shape
    half = length // 2

    barrier = pltpu.get_barrier_semaphore()
    for peer in (xp, yp, dp):
        pl.semaphore_signal(barrier, inc=1, device_id=(me, peer), device_id_type=MESH)
    pl.semaphore_wait(barrier, 3)

    def remote(src, dst, send, recv, peer):
        return pltpu.make_async_remote_copy(
            src_ref=src, dst_ref=dst, send_sem=send, recv_sem=recv,
            device_id=(me, peer), device_id_type=MESH,
        )

    def term(q):
        columns = pl.ds(pl.multiple_of(q * share, share), share)
        return jnp.dot(mixed_ref[...], weight_ref[:, columns], preferred_element_type=F32).astype(BF16)

    part_ref[2] = term(dp)
    first, second = pl.ds(0, half), pl.ds(half, half)
    hops = [
        remote(part_ref.at[2, first], hop_ref.at[0], h_send.at[0], h_recv.at[0], xp),
        remote(part_ref.at[2, second], hop_ref.at[1], h_send.at[1], h_recv.at[1], yp),
    ]
    for copy in hops:
        copy.start()
    near = []
    for i, peer in enumerate((xp, yp)):
        part_ref[i] = term(peer)
        copy = remote(part_ref.at[i], got_ref.at[i], n_send.at[i], n_recv.at[i], peer)
        copy.start()
        near.append(copy)
    kept = stream_ref[...].astype(F32) + term(tp).astype(F32)
    passed = [
        remote(hop_ref.at[0], got_ref.at[2, first], f_send.at[0], f_recv.at[0], yp),
        remote(hop_ref.at[1], got_ref.at[2, second], f_send.at[1], f_recv.at[1], xp),
    ]
    for hop, copy in zip(hops, passed):
        hop.wait_recv()
        copy.start()
    for copy in near + passed:
        copy.wait_recv()
    for i in range(3):
        kept = kept + got_ref[i].astype(F32)
    kept_ref[...] = kept
    ones = jnp.ones((8, share), F32)
    square_ref[...] = lax.dot_general(
        ones, kept * kept, (((1,), (1,)), ((), ())), precision=HIGH, preferred_element_type=F32
    )
    asks = []
    for i, peer in enumerate((xp, yp, dp)):
        copy = remote(square_ref, squares_ref.at[i], q_send.at[i], q_recv.at[i], peer)
        copy.start()
        asks.append(copy)
    for copy in asks:
        copy.wait_recv()
    squares = square_ref[...] + squares_ref[0] + squares_ref[1] + squares_ref[2]
    scale = lax.rsqrt(squares / weight_ref.shape[1] + EPS)
    pick = jnp.full((8, share), 0.125, F32)
    spread = lax.dot_general(
        scale, pick, (((0,), (0,)), ((), ())), precision=HIGH, preferred_element_type=F32
    )
    normed = (kept * spread * gain_ref[...]).astype(BF16)
    for i in range(slots_ref.shape[0]):
        slots_ref[i] = jnp.dot(place_ref[i], normed, preferred_element_type=F32).astype(BF16)
    for copy in hops + near + passed + asks:
        copy.wait_send()


def run_project(mixed, weight, stream_share, gain_share, place_of):
    n_tp = lax.axis_size("tp")
    length, share = stream_share.shape
    if n_tp != 4 or length % 32:
        partial_value = jnp.dot(mixed, weight, preferred_element_type=F32).astype(BF16)
        projected = lax.psum_scatter(partial_value, "tp", scatter_dimension=1, tiled=True)
        kept = stream_share.astype(F32) + projected.astype(F32)
        squares = lax.psum(jnp.sum(kept * kept, axis=1), "tp")
        scale = lax.rsqrt(squares / weight.shape[1] + EPS)
        normed = (kept * scale[:, None] * gain_share[None, :]).astype(BF16)
        slots = jnp.einsum("ist,td->isd", place_of, normed, preferred_element_type=F32)
        return kept, slots.astype(BF16)
    dma = lambda count: pltpu.SemaphoreType.DMA((count,))
    return pl.pallas_call(
        project_kernel,
        out_shape=(
            jax.ShapeDtypeStruct((length, share), F32),
            jax.ShapeDtypeStruct(place_of.shape[:2] + (share,), BF16),
        ),
        in_specs=[VMEM] * 5,
        out_specs=(VMEM, VMEM),
        scratch_shapes=[
            pltpu.VMEM((3, length, share), BF16),
            pltpu.VMEM((3, length, share), BF16),
            pltpu.VMEM((2, length // 2, share), BF16),
            pltpu.VMEM((8, length), F32),
            pltpu.VMEM((3, 8, length), F32),
            dma(2), dma(2), dma(2), dma(2), dma(2), dma(2), dma(3), dma(3),
        ],
        compiler_params=pltpu.CompilerParams(
            collective_id=1, has_side_effects=True, vmem_limit_bytes=48 * 2**20
        ),
        cost_estimate=pl.CostEstimate(
            flops=4 * 10**9, bytes_accessed=10**7, transcendentals=10**4
        ),
    )(mixed, weight, stream_share, gain_share[None, :], place_of)


def experts_kernel(
    n_sp, n_tp, slots_ref, gate_hbm, up_hbm, down_hbm, back_ref,
    gate_ref, up_ref, down_ref, rows_ref, hid_ref, done_ref,
    w_sem, own_sem, s_send, s_recv, x_send, x_recv, y_send, y_recv, dx_send, dx_recv, dy_send, dy_recv,
    hx_send, hx_recv, hy_send, hy_recv, hdx_send, hdx_recv, hdy_send, hdy_recv, r_send, r_recv,
):
    me = lax.axis_index("sp")
    tp = lax.axis_index("tp")
    plane, core = me // 2, me % 2
    planes = n_sp // 2
    xp = tp + 1 - 2 * (tp % 2)
    yp = (tp + 2) % 4
    experts = gate_ref.shape[0]
    half = experts // 2
    cap = rows_ref.shape[3]
    share = rows_ref.shape[4]
    width = hid_ref.shape[4]

    barrier = pltpu.get_barrier_semaphore()
    for step in range(1, n_sp):
        pl.semaphore_signal(
            barrier, inc=1, device_id=((me + step) % n_sp, tp), device_id_type=MESH
        )
    for peer in (xp, yp):
        pl.semaphore_signal(barrier, inc=1, device_id=(me, peer), device_id_type=MESH)
    pl.semaphore_wait(barrier, n_sp + 1)

    sends = []

    def remote(src, dst, send, recv, device):
        return pltpu.make_async_remote_copy(
            src_ref=src, dst_ref=dst, send_sem=send, recv_sem=recv,
            device_id=device, device_id_type=MESH,
        )

    def start(copy):
        copy.start()
        sends.append(copy)

    own = pltpu.make_async_copy(slots_ref.at[me], rows_ref.at[tp, me], own_sem.at[0])
    own.start()
    for j in range(planes):
        for c in range(2):
            if j == 0 and c == 1:
                continue
            to_core = (core + 1) % 2 if j == 0 else c
            target = ((plane - j + planes) % planes) * 2 + to_core
            start(
                remote(
                    slots_ref.at[target], rows_ref.at[tp, me], s_send.at[j * 2 + c],
                    s_recv.at[j * 2 + core], (target, tp),
                )
            )
    loads = [
        pltpu.make_async_copy(a, b, w_sem.at[i])
        for i, (a, b) in enumerate(
            ((gate_hbm, gate_ref), (up_hbm, up_ref), (down_hbm, down_ref))
        )
    ]
    for load in loads:
        load.start()

    def source(j, c):
        return ((plane + j) % planes) * 2 + c

    def exchange(buf, j, c, sems):
        s = source(j, c)
        k = j * 2 + c
        piece = buf.at[tp, s]
        start(remote(piece, piece, sems[0].at[k], sems[1].at[k], (me, xp)))
        start(remote(piece, piece, sems[2].at[k], sems[3].at[k], (me, yp)))

    def relay(buf, j, c, near, far):
        s = source(j, c)
        k = j * 2 + c
        piece = buf.at[xp, s]
        remote(piece, piece, near[0].at[k], near[1].at[k], (me, xp)).wait_recv()
        part = buf.at[xp, s, pl.ds(0, half)]
        start(remote(part, part, far[2].at[k], far[3].at[k], (me, yp)))
        piece = buf.at[yp, s]
        remote(piece, piece, near[2].at[k], near[3].at[k], (me, yp)).wait_recv()
        part = buf.at[yp, s, pl.ds(half, experts - half)]
        start(remote(part, part, far[0].at[k], far[1].at[k], (me, xp)))

    def arrive(buf, j, c, far):
        s = source(j, c)
        k = j * 2 + c
        dp = (xp + 2) % 4
        part = buf.at[dp, s, pl.ds(0, half)]
        remote(part, part, far[2].at[k], far[3].at[k], (me, yp)).wait_recv()
        part = buf.at[dp, s, pl.ds(half, experts - half)]
        remote(part, part, far[0].at[k], far[1].at[k], (me, xp)).wait_recv()

    ahead = list(range(planes))
    later = ahead[1:] + ahead[:1]

    row_near = (x_send, x_recv, y_send, y_recv)
    row_far = (dx_send, dx_recv, dy_send, dy_recv)
    hid_near = (hx_send, hx_recv, hy_send, hy_recv)
    hid_far = (hdx_send, hdx_recv, hdy_send, hdy_recv)

    def stage_a(j):
        if j == 0:
            own.wait()
            other = (core + 1) % 2
            remote(
                rows_ref.at[tp, source(0, other)], rows_ref.at[tp, source(0, other)],
                s_send.at[0], s_recv.at[other], (source(0, other), tp),
            ).wait_recv()
        for c in range(2):
            if j > 0:
                piece = rows_ref.at[tp, source(j, c)]
                remote(
                    piece, piece, s_send.at[0], s_recv.at[j * 2 + c], (source(j, c), tp)
                ).wait_recv()
            exchange(rows_ref, j, c, row_near)

    def stage_b(j):
        for c in range(2):
            relay(rows_ref, j, c, row_near, row_far)

    def stage_c(j):
        if j == later[0]:
            loads[0].wait()
            loads[1].wait()
        for c in range(2):
            arrive(rows_ref, j, c, row_far)
        first = source(j, 0)

        def one(e, carry):
            gate = jnp.zeros((2 * cap, width), F32)
            up = jnp.zeros((2 * cap, width), F32)
            for q in range(n_tp):
                x = rows_ref[q, pl.ds(first, 2), e].reshape(2 * cap, share)
                cut = slice(q * share, (q + 1) * share)
                gate = gate + jnp.dot(x, gate_ref[e, cut, :], preferred_element_type=F32)
                up = up + jnp.dot(x, up_ref[e, cut, :], preferred_element_type=F32)
            hidden = (silu(gate) * up).astype(BF16)
            hid_ref[tp, pl.ds(first, 2), e] = hidden.reshape(2, cap, width)
            return carry

        lax.fori_loop(0, experts, one, 0)
        for c in range(2):
            exchange(hid_ref, j, c, hid_near)

    def stage_d(j):
        for c in range(2):
            relay(hid_ref, j, c, hid_near, hid_far)

    keep = []

    def stage_e(j):
        if j == later[0]:
            loads[2].wait()
        for c in range(2):
            arrive(hid_ref, j, c, hid_far)
        first = source(j, 0)

        def one(e, carry):
            total = jnp.zeros((2 * cap, share), F32)
            for q in range(n_tp):
                x = hid_ref[q, pl.ds(first, 2), e].reshape(2 * cap, width)
                cut = slice(q * width, (q + 1) * width)
                total = total + jnp.dot(x, down_ref[e, cut, :], preferred_element_type=F32)
            done_ref[pl.ds(first, 2), e] = total.astype(BF16).reshape(2, cap, share)
            return carry

        lax.fori_loop(0, experts, one, 0)
        if j == 0:
            copy = pltpu.make_async_copy(done_ref.at[me], back_ref.at[me], own_sem.at[1])
            copy.start()
            keep.append(copy)
        for c in range(2):
            if j == 0 and c == 1:
                continue
            target = source(0, (core + 1) % 2) if j == 0 else source(j, c)
            start(
                remote(
                    done_ref.at[target], back_ref.at[me], r_send.at[j * 2 + c],
                    r_recv.at[j * 2 + core], (target, tp),
                )
            )

    late = 2 if planes > 1 else 1
    plan = (
        (stage_a, ahead, 0), (stage_b, ahead, 1), (stage_c, later, late + 1),
        (stage_d, later, late + 2), (stage_e, later, late + 3),
    )
    for turn in range(planes + late + 3):
        for stage, order, lag in plan:
            if 0 <= turn - lag < planes:
                stage(order[turn - lag])

    keep[0].wait()
    for j in range(planes):
        for c in range(2):
            if j == 0:
                if c == 1:
                    continue
                other = (core + 1) % 2
                origin, k = source(0, other), other
            else:
                origin, k = ((plane - j + planes) % planes) * 2 + c, j * 2 + c
            piece = back_ref.at[origin]
            remote(piece, piece, r_send.at[0], r_recv.at[k], (origin, tp)).wait_recv()
    for copy in sends:
        copy.wait_send()


def run_experts_plain(slots, expert_gate, expert_up, expert_down):
    experts, _, width = expert_gate.shape
    arrived = lax.all_to_all(slots, "sp", split_axis=0, concat_axis=0, tiled=True)
    rows = lax.all_gather(arrived, "tp", axis=3, tiled=True)
    gate = jnp.einsum("secd,edf->secf", rows, expert_gate, preferred_element_type=F32)
    up = jnp.einsum("secd,edf->secf", rows, expert_up, preferred_element_type=F32)
    hidden = lax.all_gather((jax.nn.silu(gate) * up).astype(BF16), "tp", axis=3, tiled=True)
    done = jnp.einsum("secf,efd->secd", hidden, expert_down, preferred_element_type=F32)
    return lax.all_to_all(done.astype(BF16), "sp", split_axis=0, concat_axis=0, tiled=True)


def run_experts(slots, expert_gate, expert_up, expert_down):
    n_sp, n_tp = lax.axis_size("sp"), lax.axis_size("tp")
    experts, full, width = expert_gate.shape
    share = expert_down.shape[2]
    if n_tp != 4 or n_sp % 2 or experts < 2:
        return run_experts_plain(slots, expert_gate, expert_up, expert_down)
    dma = lambda count: pltpu.SemaphoreType.DMA((count,))
    return pl.pallas_call(
        functools.partial(experts_kernel, n_sp, n_tp),
        out_shape=jax.ShapeDtypeStruct((n_sp, experts, CAP, share), BF16),
        in_specs=[VMEM, ANY, ANY, ANY],
        out_specs=VMEM,
        scratch_shapes=[
            pltpu.VMEM(expert_gate.shape, BF16),
            pltpu.VMEM(expert_up.shape, BF16),
            pltpu.VMEM(expert_down.shape, BF16),
            pltpu.VMEM((n_tp, n_sp, experts, CAP, share), BF16),
            pltpu.VMEM((n_tp, n_sp, experts, CAP, width), BF16),
            pltpu.VMEM((n_sp, experts, CAP, share), BF16),
            dma(3),
            dma(2),
        ]
        + [dma(n_sp) for _ in range(20)],
        compiler_params=pltpu.CompilerParams(
            collective_id=0, has_side_effects=True, vmem_limit_bytes=60 * 2**20
        ),
        cost_estimate=pl.CostEstimate(
            flops=10**10, bytes_accessed=2 * 10**7, transcendentals=10**6
        ),
    )(slots, expert_gate, expert_up, expert_down)


def per_device(
    stream, inner_act, gate_act, state_write, state_read, step_raw, conv_inner, conv_write, conv_read,
    step_bias, decay_log, inner_gain, out_weight, ffn_gain, expert_ids, expert_weights,
    expert_gate, expert_up, expert_down,
):
    length, inner_width = inner_act.shape
    heads = step_raw.shape[1]
    groups, state_dim = state_write.shape[1:]
    per_group = heads // groups
    head_dim = inner_width // heads
    group_width = per_group * head_dim
    write_width = groups * state_dim
    n_sp = lax.axis_size("sp")
    writes = state_write.reshape(length, write_width)
    reads = state_read.reshape(length, write_width)
    last = jnp.concatenate(
        [inner_act[length - HALO :], writes[length - HALO :], reads[length - HALO :]], axis=1
    )
    halo = lax.ppermute(last, "sp", [(i, i + 1) for i in range(n_sp - 1)])

    step_len = jax.nn.softplus(step_raw.astype(F32) + step_bias[None, :])
    rate = -jnp.exp(decay_log)
    lower = jnp.tril(jnp.ones((length, length), F32))
    cumul = jnp.dot(lower, step_len * rate[None, :], precision=HIGH)
    total = cumul[-1]
    to_end = jnp.exp(total[None, :] - cumul) * step_len
    by_group = lambda a: a.reshape(length, groups, per_group).transpose(1, 0, 2)
    cum_g = by_group(cumul)
    cum_t = cum_g.transpose(0, 2, 1)
    step_t = by_group(step_len).transpose(0, 2, 1)
    end_g = by_group(to_end)
    sum_g = total.reshape(groups, 1, per_group)
    state_rows = group_width + -(-3 * per_group // 16) * 16

    col = lambda rows, cols: pl.BlockSpec((rows, cols), lambda g: (0, g))
    lead = lambda a: pl.BlockSpec((1,) + a.shape[1:], lambda g: (g, 0, 0))
    taps = conv_inner.shape[0]
    params = pltpu.CompilerParams(vmem_limit_bytes=48 * 2**20)
    xs, bw, cr, state = pl.pallas_call(
        functools.partial(conv_kernel, per_group),
        grid=(groups,),
        out_shape=(
            jax.ShapeDtypeStruct((length, inner_width), BF16),
            jax.ShapeDtypeStruct((length, write_width), BF16),
            jax.ShapeDtypeStruct((length, write_width), BF16),
            jax.ShapeDtypeStruct((groups, state_rows, state_dim), BF16),
        ),
        in_specs=[
            col(length, group_width), col(length, state_dim), col(length, state_dim),
            col(HALO, group_width), col(HALO, state_dim), col(HALO, state_dim),
            col(taps, group_width), col(taps, state_dim), col(taps, state_dim), lead(end_g),
            lead(sum_g),
        ],
        out_specs=(
            col(length, group_width), col(length, state_dim), col(length, state_dim),
            pl.BlockSpec((1, state_rows, state_dim), lambda g: (g, 0, 0)),
        ),
        scratch_shapes=[pltpu.VMEM((length + HALO, max(group_width, state_dim)), F32)],
        compiler_params=params,
        cost_estimate=pl.CostEstimate(flops=10**9, bytes_accessed=10**7, transcendentals=10**6),
    )(
        inner_act, writes, reads,
        halo[:, :inner_width], halo[:, inner_width : inner_width + write_width],
        halo[:, inner_width + write_width :],
        conv_inner, conv_write.reshape(taps, write_width), conv_read.reshape(taps, write_width), end_g, sum_g,
    )
    states = lax.all_gather(state, "sp")

    inside = pl.pallas_call(
        functools.partial(inside_kernel, per_group),
        grid=(groups,),
        out_shape=jax.ShapeDtypeStruct((length, inner_width), F32),
        in_specs=[
            col(length, group_width), col(length, state_dim), col(length, state_dim),
            lead(cum_g), lead(cum_t), lead(step_t),
        ],
        out_specs=col(length, group_width),
        compiler_params=params,
        cost_estimate=pl.CostEstimate(
            flops=4 * 10**9, bytes_accessed=10**7, transcendentals=3 * 10**6
        ),
    )(xs, bw, cr, cum_g, cum_t, step_t)

    mixed_inner = pl.pallas_call(
        functools.partial(outside_kernel, per_group),
        grid=(groups,),
        out_shape=jax.ShapeDtypeStruct((length, inner_width), BF16),
        in_specs=[
            col(length, group_width), col(length, state_dim),
            pl.BlockSpec((n_sp, 1, state_rows, state_dim), lambda g: (0, g, 0, 0)),
            lead(cum_g), col(length, group_width), col(1, group_width),
        ],
        out_specs=col(length, group_width),
        compiler_params=params,
        cost_estimate=pl.CostEstimate(flops=10**9, bytes_accessed=10**7, transcendentals=10**6),
    )(inside, cr, states, cum_g, gate_act, inner_gain[None, :])

    local_experts = expert_gate.shape[0]
    expert_count = local_experts * n_sp
    ids = expert_ids.reshape(-1)
    onehot = (ids[:, None] == jnp.arange(expert_count, dtype=jnp.int32)[None, :]).astype(BF16)
    pairs = ids.shape[0]
    before = jnp.tril(jnp.ones((pairs, pairs), BF16), -1)
    earlier = jnp.dot(before, onehot, preferred_element_type=F32)
    slot_of = jnp.sum(earlier * onehot.astype(F32), axis=1).astype(jnp.int32)
    target = (ids * CAP + slot_of).reshape(length, TOPK)
    slots = jnp.arange(expert_count * CAP, dtype=jnp.int32)
    named = [target[:, k][:, None] == slots[None, :] for k in range(TOPK)]
    placed = [slots[:, None] == target[:, k][None, :] for k in range(TOPK)]
    place_of = functools.reduce(jnp.logical_or, placed).astype(BF16)
    mix = functools.reduce(
        jnp.add, [jnp.where(n, expert_weights[:, k : k + 1], 0.0) for k, n in enumerate(named)]
    )
    mix_high = mix.astype(BF16)
    mix_low = (mix - mix_high.astype(F32)).astype(BF16)

    out_width = expert_down.shape[2]
    own_start = lax.axis_index("tp") * out_width
    stream_share = lax.dynamic_slice_in_dim(stream, own_start, out_width, 1)
    gain_share = lax.dynamic_slice_in_dim(ffn_gain, own_start, out_width, 0)
    kept, outgoing = run_project(
        mixed_inner, out_weight, stream_share, gain_share, place_of.reshape(n_sp, -1, length)
    )
    back = run_experts(
        outgoing.reshape(n_sp, local_experts, CAP, out_width), expert_gate, expert_up, expert_down
    )
    results = back.reshape(expert_count * CAP, out_width)
    moe = jnp.dot(mix_high, results, preferred_element_type=F32) + jnp.dot(
        mix_low, results, preferred_element_type=F32
    )
    return (kept + moe).astype(BF16)


def solution(mesh):
    return jax.shard_map(
        per_device,
        mesh=mesh,
        in_specs=(
            P("sp", None), P("sp", "tp"), P("sp", "tp"), P("sp", "tp", None), P("sp", "tp", None),
            P("sp", "tp"), P(None, "tp"), P(None, "tp", None), P(None, "tp", None), P("tp"), P("tp"),
            P("tp"), P("tp", None), P(), P("sp", None), P("sp", None), P("sp", None, "tp"),
            P("sp", None, "tp"), P("sp", None, "tp"),
        ),
        out_specs=P("sp", "tp"),
        check_vma=False,
    )
```
